32 devices in a mesh: grp: 2 (over y), sp: 4 (over z), tp: 4 (over x, core).
Axes of the slice: x: 2, y: 2, z: 4, core: 2. Of those that a mesh axis runs over, the one named last changes fastest.
Arguments:
- carryover_vector: bfloat16 [2048, 2048], P(('grp', 'sp', 'tp')), parts along dimension 0, may hold values from -6 to 6
- channel_source_entries: bfloat16 [2048, 1024], P(('grp', 'sp'), 'tp'), parts along dimension 0, may hold values from -6 to 6
- final_modulation_vector: bfloat16 [2048, 1024], P(('grp', 'sp'), 'tp'), parts along dimension 0, may hold values from -54 to 54
- entering_basis_matrix: bfloat16 [2048, 512], P(('grp', 'sp'), 'tp'), parts along dimension 0, may hold values from -6 to 6
- readout_basis_matrix: bfloat16 [2048, 512], P(('grp', 'sp'), 'tp'), parts along dimension 0, may hold values from -6 to 6
- raw_stride_amount: float32 [2048, 16], P(('grp', 'sp'), 'tp'), parts along dimension 0, may hold values from -6 to 5
- extra_log_attenuation: float32 [2048, 16], P(('grp', 'sp'), 'tp'), parts along dimension 0, may hold values from -1.4 to 0
- channel_fading_rate: float32 [16], P('tp'), may hold values from 0 to 0.1, as said below
- channel_source_kernel: float32 [4, 1024], P(None, 'tp'), may hold values from -3 to 3
- entering_basis_kernel: float32 [4, 512], P(None, 'tp'), may hold values from -3 to 3
- readout_basis_kernel: float32 [4, 512], P(None, 'tp'), may hold values from -3 to 3
- modulated_rescaling_vector: float32 [1024], replicated, may hold values from 0.1 to 1.9
- blender_final_matrix: bfloat16 [1024, 2048], replicated, may hold values from -0.1875 to 0.1875
- specialist_rescaling_vector: float32 [2048], replicated, may hold values from 0.1 to 1.9
- specialist_gating_matrices: bfloat16 [8, 2048, 1024], P('sp', None, 'tp'), may hold values from -0.125 to 0.125
- widening_matrices: bfloat16 [8, 2048, 1024], P('sp', None, 'tp'), may hold values from -0.125 to 0.125
- contracting_matrices: bfloat16 [8, 1024, 2048], P('sp', 'tp'), may hold values from -0.1875 to 0.1875
- assigned_specialist_ids: int32 [2048, 2], P(('grp', 'sp')), parts along dimension 0, may hold values from 0 to 7, as said below
- specialist_choice_affinity: float32 [2048, 2], P(('grp', 'sp', 'tp')), parts along dimension 0, may hold values from -6 to 6
- cluster_chance: float32 [2048], P(('grp', 'sp', 'tp')), parts along dimension 0, may hold values from 0.25 to 1
Outputs:
- layer_out: bfloat16 [2048, 2048], P(('grp', 'sp', 'tp')), parts along dimension 0
The draws below stay inside these ranges and needn't reach their ends.
There are 2 independent parts, one for each index of `grp`. The reference program is written for one: setup_inputs(seed, part) draws one part's arguments, and reference() takes and returns one part's arrays. A program takes and returns all parts, laid end to end along the dimension named above; an argument that names none is the same for every part. Nothing has to cross between parts.
Inputs may be any that keep to these rules, and one draw needn't show every extreme that they name: `assigned_specialist_ids`: each row names 2 different experts of one group: the experts g * 2 to (g + 1) * 2 - 1 for one g below 4. In each aligned block of 64 rows (the rows of one device) no expert is named by more than 32 rows, and every expert of one group, the same group in all blocks, is named by exactly 32 rows of every block. `channel_fading_rate`: positive.
All inputs are finite; a program needn't handle non-finite values.
Results may differ from the reference program's by a relative error of at most 0.015.
Values may be sent and summed in bfloat16 or wider, within the bound.
No kernel may reach another device: no remote copies, remote signals or barrier semaphores. Data moves between devices by JAX's collectives and lax.ppermute only.
A program may use at most 64 MiB of HBM per device.

```python
import jax
import jax.numpy as jnp
from jax import lax

D = 2048
HEADS = 16
HEAD_DIM = 64
GROUPS_BC = 4
STATE = 128
CONV = 4
BLOCK = 64
FF = 1024
EGROUPS = 4
TOPK = 2
SEG_TOK = 256
D_SSD = 1024
ROWS = 64
TOKENS = 1024
EXPERTS = 8
CAP = 32
N_TP = 4


def draw_final_modulation_vector(key, part):
    row_key, column_key, base_key = jax.random.split(jax.random.fold_in(key, 7), 3)
    row_scale = jnp.exp(jax.random.uniform(row_key, (TOKENS, 1), jnp.float32, jnp.log(0.3), jnp.log(3.0)))
    column = jnp.arange(D_SSD, dtype=jnp.float32)[None, :] / D_SSD
    jitter = jnp.exp(jax.random.uniform(column_key, (1, D_SSD), jnp.float32, jnp.log(0.6), jnp.log(1.5)))
    base = jnp.clip(jax.random.normal(base_key, (TOKENS, D_SSD), jnp.float32), -4.0, 4.0)
    column_scale = jnp.exp(column * jnp.log(3.0)) * jitter
    return (base * row_scale * column_scale).astype(jnp.bfloat16)


def draw_raw_stride_amount(key, part):
    jitter_key, level_key = jax.random.split(jax.random.fold_in(key, 11))
    segments = TOKENS // SEG_TOK
    levels = jax.random.uniform(level_key, (segments, 1, 1), jnp.float32, -1.5, 1.0)
    jitter = jnp.clip(jax.random.normal(jitter_key, (segments, SEG_TOK, HEADS), jnp.float32), -4.5, 4.0)
    return (jitter + levels).reshape(TOKENS, HEADS)


def draw_channel_fading_rate(key, part):
    pick_key, slow_key, fast_key = jax.random.split(jax.random.fold_in(key, 13), 3)
    slow_share = 0.5
    is_slow = jax.random.uniform(pick_key, (HEADS,), jnp.float32) < slow_share
    slow_rates = jnp.exp(jax.random.uniform(slow_key, (HEADS,), jnp.float32, jnp.log(0.1 / TOKENS), jnp.log(1.0 / TOKENS)))
    fast_rates = jnp.exp(jax.random.uniform(fast_key, (HEADS,), jnp.float32, jnp.log(0.03), jnp.log(0.1)))
    return jnp.where(is_slow, slow_rates, fast_rates)


def draw_extra_log_attenuation(key, part):
    place_key, strength_key = jax.random.split(jax.random.fold_in(key, 17))
    places = jax.random.randint(place_key, (2, 1, HEADS), 0, TOKENS)
    strengths = jax.random.uniform(strength_key, (2, 1, HEADS), jnp.float32, 0.22, 0.69)
    positions = jnp.arange(TOKENS, dtype=jnp.int32)[None, :, None]
    return -jnp.sum(jnp.where(positions == places, strengths, 0.0), axis=0)


def draw_assigned_specialist_ids(key, part):
    blocks = TOKENS // ROWS
    per_group = EXPERTS // EGROUPS
    busy_rows = CAP * per_group // TOPK
    busy_key, other_key, order_key, deal_key = jax.random.split(jax.random.fold_in(key, 19), 4)
    busy_group = jax.random.randint(busy_key, (), 0, EGROUPS)
    others = jax.random.randint(other_key, (blocks, ROWS - busy_rows), 0, EGROUPS - 1)
    others = others + (others >= busy_group).astype(jnp.int32)
    groups = jnp.concatenate([jnp.full((blocks, busy_rows), busy_group, jnp.int32), others], axis=1)
    orders = jax.vmap(lambda subkey: jax.random.permutation(subkey, ROWS))(jax.random.split(order_key, blocks))
    groups = jnp.take_along_axis(groups, orders, axis=1)
    member = (groups[..., None] == jnp.arange(EGROUPS, dtype=jnp.int32)).astype(jnp.int32)
    ranking = jnp.sum((jnp.cumsum(member, axis=1) - member) * member, axis=2)
    dealing = jax.vmap(lambda subkey: jax.random.permutation(subkey, per_group))(jax.random.split(deal_key, blocks * EGROUPS)).reshape(blocks, EGROUPS, per_group)
    chosen = dealing[jnp.arange(blocks)[:, None], groups]
    first_place = TOPK * ranking % per_group
    first_pick = jnp.take_along_axis(chosen, first_place[..., None], axis=2)[..., 0]
    second_pick = jnp.take_along_axis(chosen, (first_place + 1)[..., None], axis=2)[..., 0]
    group_base = groups * per_group
    picked = jnp.stack([group_base + first_pick, group_base + second_pick], axis=-1)
    return picked.reshape(TOKENS, TOPK).astype(jnp.int32)


def block_levels(own_key, extent, cuts, low, top_value):
    def one(position, parts):
        steps = jax.random.uniform(jax.random.fold_in(jax.random.fold_in(own_key, 6), position), (parts,), jnp.float32, low / len(cuts), top_value / len(cuts))
        return jnp.repeat(jnp.exp(steps), extent[position] // parts).reshape((-1,) + (1,) * (len(extent) - position - 1))

    level = one(*cuts[0])
    for cut in cuts[1:]:
        level = level * one(*cut)
    return level


def centred(own_key, shape, width, limit, shards=(), kind=jnp.bfloat16):
    values = jax.random.normal(own_key, shape, jnp.float32) * width
    if len(shards) > 0:
        values = block_levels(own_key, shape, shards, -0.22, 0.18) * values
    return jnp.clip(values, min=-limit, max=limit).astype(kind)


def setup_inputs(seed: int = 0, part: int = 0) -> dict:
    streams_of = jax.random.split(jax.random.key(seed), 21)
    own_keys = jax.random.split(jax.random.fold_in(streams_of[20], part), 21)
    carryover_vector = centred(own_keys[0], (TOKENS, D), 1.0, 6.0, ((0, 16),))
    channel_source_entries = centred(own_keys[1], (TOKENS, D_SSD), 1.0, 6.0, ((0, 4), (1, 4)))
    final_modulation_vector = draw_final_modulation_vector(jax.random.fold_in(jax.random.fold_in(streams_of[20], part), 71), part)
    entering_basis_matrix = centred(own_keys[3], (TOKENS, GROUPS_BC * STATE), 1.0, 6.0, ((0, 4), (1, 4)))
    readout_basis_matrix = centred(own_keys[4], (TOKENS, GROUPS_BC * STATE), 1.0, 6.0, ((0, 4), (1, 4)))
    raw_stride_amount = draw_raw_stride_amount(jax.random.fold_in(jax.random.fold_in(streams_of[20], part), 71), part)
    extra_log_attenuation = draw_extra_log_attenuation(jax.random.fold_in(jax.random.fold_in(streams_of[20], part), 71), part)
    channel_fading_rate = draw_channel_fading_rate(jax.random.fold_in(streams_of[20], 71), part)
    channel_source_kernel = centred(streams_of[8], (CONV, D_SSD), CONV ** -0.5, 3.0, ((1, 4),), jnp.float32)
    entering_basis_kernel = centred(streams_of[9], (CONV, GROUPS_BC * STATE), CONV ** -0.5, 3.0, ((1, 4),), jnp.float32)
    readout_basis_kernel = centred(streams_of[10], (CONV, GROUPS_BC * STATE), CONV ** -0.5, 3.0, ((1, 4),), jnp.float32)
    modulated_rescaling_vector = jnp.clip(1.0 + 0.18 * jax.random.normal(streams_of[11], (D_SSD,), jnp.float32), 0.1, 1.9)
    blender_final_matrix = centred(streams_of[12], (D_SSD, D), D_SSD ** -0.5, 0.1875)
    specialist_rescaling_vector = jnp.clip(1.0 + 0.18 * jax.random.normal(streams_of[13], (D,), jnp.float32), 0.1, 1.9)
    specialist_gating_matrices = centred(streams_of[14], (EXPERTS, D, FF), D ** -0.5, 0.125, ((0, 4), (2, 4)))
    widening_matrices = centred(streams_of[15], (EXPERTS, D, FF), D ** -0.5, 0.125, ((0, 4), (2, 4)))
    contracting_matrices = centred(streams_of[16], (EXPERTS, FF, D), FF ** -0.5, 0.1875, ((0, 4), (1, 4)))
    assigned_specialist_ids = draw_assigned_specialist_ids(jax.random.fold_in(jax.random.fold_in(streams_of[20], part), 71), part)
    specialist_choice_affinity = centred(own_keys[18], (TOKENS, TOPK), 1.5, 6.0, ((0, 16),), jnp.float32)
    cluster_chance = jnp.clip(0.25 + 0.75 * jax.random.uniform(own_keys[19], (TOKENS,), jnp.float32) ** block_levels(own_keys[19], (TOKENS,), ((0, 16),), -0.2, 0.2), 0.25, 1.0)
    return dict(carryover_vector=carryover_vector, channel_source_entries=channel_source_entries, final_modulation_vector=final_modulation_vector, entering_basis_matrix=entering_basis_matrix, readout_basis_matrix=readout_basis_matrix, raw_stride_amount=raw_stride_amount, extra_log_attenuation=extra_log_attenuation, channel_fading_rate=channel_fading_rate, channel_source_kernel=channel_source_kernel, entering_basis_kernel=entering_basis_kernel, readout_basis_kernel=readout_basis_kernel, modulated_rescaling_vector=modulated_rescaling_vector, blender_final_matrix=blender_final_matrix, specialist_rescaling_vector=specialist_rescaling_vector, specialist_gating_matrices=specialist_gating_matrices, widening_matrices=widening_matrices, contracting_matrices=contracting_matrices, assigned_specialist_ids=assigned_specialist_ids, specialist_choice_affinity=specialist_choice_affinity, cluster_chance=cluster_chance)


EPS = 1e-06
HIGHEST = lax.Precision.HIGHEST

def causal_conv(signal, weights):
    kernel_len = weights.shape[0]
    length = signal.shape[0]
    padded = jnp.pad(signal.astype(jnp.float32), ((kernel_len - 1, 0), (0, 0)))
    accumulated = jnp.zeros((length, signal.shape[1]), jnp.float32)
    for offset in range(kernel_len):
        accumulated = accumulated + weights[offset][None, :] * padded[offset:offset + length]
    return jax.nn.silu(accumulated)

def state_space(scaled_in, log_attenuation, keys_b, queries_c):
    blocks = scaled_in.shape[0] // BLOCK
    per_group = HEADS // GROUPS_BC
    scaled_in = scaled_in.reshape(blocks, BLOCK, GROUPS_BC, per_group, HEAD_DIM)
    log_attenuation = log_attenuation.reshape(blocks, BLOCK, GROUPS_BC, per_group)
    keys_b = keys_b.reshape(blocks, BLOCK, GROUPS_BC, STATE)
    queries_c = queries_c.reshape(blocks, BLOCK, GROUPS_BC, STATE)
    lower_mask = jnp.tril(jnp.ones((BLOCK, BLOCK), dtype=bool))

    def advance(carried, pieces):
        block_in, block_log, block_b, block_c = pieces
        running = jnp.cumsum(block_log, axis=0)
        between = running[:, None] - running[None, :]
        decays = jnp.exp(jnp.where(lower_mask[:, :, None, None], between, -jnp.inf))
        scores = jnp.einsum('lgn,sgn->lsg', block_c, block_b, precision=HIGHEST)
        inside = jnp.einsum('lsg,lsgr,sgrp->lgrp', scores, decays, block_in, precision=HIGHEST)
        outside = jnp.einsum('lgn,grpn,lgr->lgrp', block_c, carried, jnp.exp(running), precision=HIGHEST)
        remain = jnp.exp(running[-1][None] - running)
        updated = carried * jnp.exp(running[-1])[:, :, None, None] + jnp.einsum('sgn,sgr,sgrp->grpn', block_b, remain, block_in, precision=HIGHEST)
        return (updated, inside + outside)
    initial = jnp.zeros((GROUPS_BC, per_group, HEAD_DIM, STATE), jnp.float32)
    _, outputs = lax.scan(advance, initial, (scaled_in, log_attenuation, keys_b, queries_c))
    return outputs.reshape(blocks * BLOCK, HEADS, HEAD_DIM)

def reference(carryover_vector, channel_source_entries, final_modulation_vector, entering_basis_matrix, readout_basis_matrix, raw_stride_amount, extra_log_attenuation, channel_fading_rate, channel_source_kernel, entering_basis_kernel, readout_basis_kernel, modulated_rescaling_vector, blender_final_matrix, specialist_rescaling_vector, specialist_gating_matrices, widening_matrices, contracting_matrices, assigned_specialist_ids, specialist_choice_affinity, cluster_chance):
    length = carryover_vector.shape[0]
    inputs_x = causal_conv(channel_source_entries, channel_source_kernel)
    keys_b = causal_conv(entering_basis_matrix, entering_basis_kernel)
    queries_c = causal_conv(readout_basis_matrix, readout_basis_kernel)
    channel_stride_amount = jax.nn.softplus(raw_stride_amount)
    log_attenuation = extra_log_attenuation - channel_fading_rate[None, :] * channel_stride_amount
    heads_x = inputs_x.reshape(length, HEADS, HEAD_DIM)
    mixed = state_space(heads_x * channel_stride_amount[:, :, None], log_attenuation, keys_b, queries_c)
    gated = mixed.reshape(length, D_SSD) * jax.nn.silu(final_modulation_vector.astype(jnp.float32))
    normed = (gated * lax.rsqrt(lax.optimization_barrier(jnp.mean(gated * gated, axis=1, keepdims=True)) + EPS) * modulated_rescaling_vector[None, :]).astype(jnp.bfloat16)
    middle = (carryover_vector.astype(jnp.float32) + jnp.dot(normed, blender_final_matrix, preferred_element_type=jnp.float32)).astype(jnp.bfloat16)
    middle_wide = middle.astype(jnp.float32)
    expert_input = (middle_wide * lax.rsqrt(lax.optimization_barrier(jnp.mean(middle_wide * middle_wide, axis=1, keepdims=True)) + EPS) * specialist_rescaling_vector[None, :]).astype(jnp.bfloat16)
    assigned = assigned_specialist_ids.reshape(-1)
    count_all = assigned.shape[0]
    member = (assigned[:, None] == jnp.arange(EXPERTS, dtype=jnp.int32)[None, :]).astype(jnp.int32)
    ranking = lax.optimization_barrier(jnp.sum((jnp.cumsum(member, axis=0) - member) * member, axis=1))
    slot_count = length // ROWS * CAP
    table = jnp.full((EXPERTS, slot_count), -1, jnp.int32).at[assigned, ranking].set(jnp.arange(count_all, dtype=jnp.int32))
    lifted = jnp.exp(specialist_choice_affinity)
    shares = (cluster_chance[:, None] * lifted / lax.optimization_barrier(jnp.sum(lifted, axis=1, keepdims=True))).reshape(-1)
    quarter = FF // N_TP

    def expert_pass(combined, expert_index):
        slot_ids = table[expert_index]
        is_live = slot_ids >= 0
        safe_ids = jnp.maximum(slot_ids, 0)
        token_ids = safe_ids // TOPK
        chosen = jnp.take(expert_input, token_ids, axis=0)
        gate_value = jnp.dot(chosen, specialist_gating_matrices[expert_index], preferred_element_type=jnp.float32)
        up_value = jnp.dot(chosen, widening_matrices[expert_index], preferred_element_type=jnp.float32)
        hidden = (jax.nn.silu(gate_value) * up_value).astype(jnp.bfloat16)
        down_rows = contracting_matrices[expert_index]
        summed = jnp.zeros((slot_count, D), jnp.float32)
        for part_index in range(N_TP):
            piece_sum = jnp.dot(hidden[:, part_index * quarter:(part_index + 1) * quarter], down_rows[part_index * quarter:(part_index + 1) * quarter], preferred_element_type=jnp.float32).astype(jnp.bfloat16)
            summed = summed + lax.optimization_barrier(piece_sum).astype(jnp.float32)
        result = lax.optimization_barrier(summed.astype(jnp.bfloat16)).astype(jnp.float32)
        weight_column = jnp.where(is_live, shares[safe_ids], 0.0)
        return (combined.at[token_ids].add(weight_column[:, None] * result), None)
    combined, _ = lax.scan(expert_pass, jnp.zeros((length, D), jnp.float32), jnp.arange(EXPERTS, dtype=jnp.int32))
    return (middle_wide + combined).astype(jnp.bfloat16)
```

```python
import jax
import jax.numpy as jnp
from jax import lax
from jax.sharding import PartitionSpec as P

HEAD_DIM = 64
STATE = 128
BLOCK = 64
EGROUPS = 4
MANY = 8


EPS = 1e-06
HIGHEST = lax.Precision.HIGHEST


def shifted(x, axis, by):
    size = lax.axis_size(axis)
    return lax.ppermute(x, axis, [(i, (i + by) % size) for i in range(size)])


def flipped(x, axis, bit):
    return lax.ppermute(x, axis, [(i, i ^ bit) for i in range(lax.axis_size(axis))])


def incoming_states(own_state, own_decay):
    size, index = (lax.axis_size("sp"), lax.axis_index("sp"))
    groups, per_group, width, entries = own_state.shape
    heads = groups * per_group
    rows = heads * width
    extra = -(-heads // 16) * 16
    decay_rows = jnp.broadcast_to(own_decay.reshape(heads, 1), (heads, entries))
    packed = jnp.concatenate(
        [
            own_state.reshape(rows, entries).astype(jnp.bfloat16),
            jnp.pad(decay_rows, ((0, extra - heads), (0, 0))).astype(jnp.bfloat16),
        ]
    )
    if size <= MANY:
        behind = [from_behind(packed, "sp", by) for by in range(1, size)]
    else:
        everything = lax.all_gather(packed, "sp")
        behind = [
            jnp.where(index >= by, jnp.take(everything, jnp.maximum(index - by, 0), axis=0), 0)
            for by in range(1, size)
        ]
    total = jnp.zeros((heads, width, entries), jnp.float32)
    for piece in reversed(behind):
        decay = piece[rows : rows + heads].astype(jnp.float32)
        state = piece[:rows].reshape(heads, width, entries).astype(jnp.float32)
        total = total * decay[:, None, :] + state
    return total.reshape(own_state.shape)


def from_behind(x, axis, by):
    size = lax.axis_size(axis)
    pairs = [(i, i + by) for i in range(size) if 0 <= i + by < size]
    return lax.ppermute(x, axis, pairs)


def causal_conv(signal, earlier, weights):
    kernel_len = weights.shape[0]
    length = signal.shape[0]
    joined = jnp.concatenate([earlier, signal], axis=0).astype(jnp.float32)
    accumulated = jnp.zeros((length, signal.shape[1]), jnp.float32)
    for offset in range(kernel_len):
        accumulated = accumulated + weights[offset][None, :] * joined[offset : offset + length]
    return jax.nn.silu(accumulated)


def device_states(scaled_in, log_attenuation, keys_b, queries_c, groups_here):
    length = scaled_in.shape[0]
    blocks = length // BLOCK
    per_group = scaled_in.shape[1] // groups_here
    scaled_in = scaled_in.reshape(blocks, BLOCK, groups_here, per_group, HEAD_DIM)
    log_attenuation = log_attenuation.reshape(blocks, BLOCK, groups_here, per_group)
    keys_b = keys_b.reshape(blocks, BLOCK, groups_here, STATE)
    queries_c = queries_c.reshape(blocks, BLOCK, groups_here, STATE)
    running = jnp.cumsum(log_attenuation, axis=1)
    lower_mask = jnp.tril(jnp.ones((BLOCK, BLOCK), dtype=bool))
    between = running[:, :, None] - running[:, None, :]
    decays = jnp.exp(jnp.where(lower_mask[None, :, :, None, None], between, -jnp.inf))
    scores = jnp.einsum("blgn,bsgn->blsg", queries_c, keys_b, precision=HIGHEST)
    inside = jnp.einsum("blsg,blsgr,bsgrp->blgrp", scores, decays, scaled_in, precision=HIGHEST)
    totals = running[:, -1]
    remain = jnp.exp(totals[:, None] - running)
    block_states = jnp.einsum(
        "bsgn,bsgr,bsgrp->bgrpn", keys_b, remain, scaled_in, precision=HIGHEST
    )

    def advance(carried, pieces):
        return (carried * jnp.exp(pieces[1])[..., None, None] + pieces[0], carried)

    initial = jnp.zeros(block_states.shape[1:], jnp.float32)
    own_state, entering = lax.scan(advance, initial, (block_states, totals))
    own_decay = jnp.exp(jnp.sum(totals, axis=0))
    incoming = incoming_states(own_state, own_decay)
    preceding = jnp.exp(jnp.cumsum(totals, axis=0) - totals)
    entering = entering + preceding[..., None, None] * incoming[None]
    outside = jnp.einsum(
        "blgn,bgrpn,blgr->blgrp", queries_c, entering, jnp.exp(running), precision=HIGHEST
    )
    return (inside + outside).reshape(length, -1)


def sp_exchange(pieces, sign):
    size, index = (lax.axis_size("sp"), lax.axis_index("sp"))
    if size <= MANY:
        return [pieces[0]] + [shifted(pieces[m], "sp", sign * m) for m in range(1, size)]
    places = jnp.arange(size, dtype=jnp.int32)
    sent = jnp.take(pieces, (sign * (places - index)) % size, axis=0)
    came = lax.all_to_all(sent, "sp", split_axis=0, concat_axis=0, tiled=True)
    came = jnp.take(came, (index - sign * places) % size, axis=0)
    return [came[m] for m in range(size)]


def to_experts(pieces):
    return sp_exchange(pieces, 1)


def from_experts(pieces):
    return sp_exchange(pieces, -1)


def near_order(size):
    order, bit = ([0], size // 2)
    while bit:
        order = order + [m | bit for m in order]
        bit //= 2
    return order


def gather_near(x, axis):
    bit = lax.axis_size("tp") // 2
    blocks, width = ([x], x.shape[axis])
    while bit:
        came = flipped(jnp.concatenate(blocks, axis=axis), "tp", bit)
        blocks = blocks + [
            lax.slice_in_dim(came, i * width, (i + 1) * width, axis=axis)
            for i in range(len(blocks))
        ]
        bit //= 2
    return blocks


def ordered(blocks, index):
    by = dict(zip(near_order(len(blocks)), blocks))
    bit = 1
    while bit < len(blocks):
        here = (index & bit) != 0
        by = {m: jnp.where(here, by[m ^ bit], by[m]) for m in by}
        bit *= 2
    return [by[m] for m in range(len(blocks))]


def per_device(
    carryover_vector,
    channel_source_entries,
    final_modulation_vector,
    entering_basis_matrix,
    readout_basis_matrix,
    raw_stride_amount,
    extra_log_attenuation,
    channel_fading_rate,
    channel_source_kernel,
    entering_basis_kernel,
    readout_basis_kernel,
    modulated_rescaling_vector,
    blender_final_matrix,
    specialist_rescaling_vector,
    specialist_gating_matrices,
    widening_matrices,
    contracting_matrices,
    assigned_specialist_ids,
    specialist_choice_affinity,
    cluster_chance,
):
    length, head_cols = channel_source_entries.shape
    row_count, model_width = carryover_vector.shape
    heads_here = channel_fading_rate.shape[0]
    state_cols = entering_basis_matrix.shape[1]
    groups_here = state_cols // STATE
    sp_count, sp_index = (lax.axis_size("sp"), lax.axis_index("sp"))
    tp_count, tp_index = (lax.axis_size("tp"), lax.axis_index("tp"))
    rim_rows = channel_source_kernel.shape[0] - 1
    local_experts = specialist_gating_matrices.shape[0]
    experts = sp_count * local_experts
    picks = assigned_specialist_ids.shape[1]
    capacity = 2 * row_count * picks // experts
    slots = min(local_experts * capacity, capacity * (experts // EGROUPS) // picks)

    everything = jnp.concatenate(
        [channel_source_entries, entering_basis_matrix, readout_basis_matrix], axis=1
    )
    neighbours = from_behind(everything[length - rim_rows :], "sp", 1)

    member = jnp.any(
        ((assigned_specialist_ids // local_experts - sp_index) % sp_count)[:, :, None]
        == jnp.arange(sp_count, dtype=jnp.int32),
        axis=1,
    )
    row = jnp.arange(length, dtype=jnp.int32)
    earlier = (row[:, None] > row[None, :]) & (
        row[:, None] // row_count == row[None, :] // row_count
    )
    rank = jnp.dot(
        earlier.astype(jnp.bfloat16),
        member.astype(jnp.bfloat16),
        preferred_element_type=jnp.float32,
    ).astype(jnp.int32)
    place = jnp.where(member, rank + (row // row_count * slots)[:, None], -1)
    own_place = lax.dynamic_slice_in_dim(
        jnp.where(member, rank, -1), tp_index * row_count, row_count, 0
    )
    pick_own = (
        own_place.T[:, None, :] == jnp.arange(slots, dtype=jnp.int32)[None, :, None]
    ).astype(jnp.bfloat16)
    pick_own = pick_own.reshape(sp_count * slots, row_count)
    pick_all = (
        place.T[:, None, :] == jnp.arange(tp_count * slots, dtype=jnp.int32)[None, :, None]
    ).astype(jnp.bfloat16)

    lifted = jnp.exp(specialist_choice_affinity)
    shares = cluster_chance[:, None] * lifted / jnp.sum(lifted, axis=1, keepdims=True)
    shares_high = shares.astype(jnp.bfloat16)
    shares_low = (shares - shares_high.astype(jnp.float32)).astype(jnp.bfloat16)
    own_ids = lax.dynamic_slice_in_dim(assigned_specialist_ids, tp_index * row_count, row_count, 0)
    notes = jnp.concatenate([shares_high, shares_low, own_ids.astype(jnp.bfloat16)], axis=1)
    notes = jnp.pad(notes, ((0, 0), (0, 128 - 3 * picks)))
    early = jnp.dot(
        pick_own,
        jnp.concatenate([carryover_vector, notes], axis=1),
        preferred_element_type=jnp.float32,
    ).astype(jnp.bfloat16)
    early = to_experts(early.reshape(sp_count, slots, model_width + 128))
    early = gather_near(jnp.concatenate(early, axis=0), 0)
    carried = jnp.concatenate(early, axis=0)

    weights = jnp.concatenate(
        [channel_source_kernel, entering_basis_kernel, readout_basis_kernel], axis=1
    )
    mixed_in = causal_conv(everything, neighbours, weights)
    inputs_x = mixed_in[:, :head_cols]
    keys_b = mixed_in[:, head_cols : head_cols + state_cols]
    queries_c = mixed_in[:, head_cols + state_cols :]
    channel_stride_amount = jax.nn.softplus(raw_stride_amount)
    log_attenuation = extra_log_attenuation - channel_fading_rate[None, :] * channel_stride_amount
    heads_x = inputs_x.reshape(length, heads_here, HEAD_DIM)
    mixed = device_states(
        heads_x * channel_stride_amount[:, :, None], log_attenuation, keys_b, queries_c, groups_here
    )
    gated = (mixed * jax.nn.silu(final_modulation_vector.astype(jnp.float32))).astype(jnp.bfloat16)

    routed = jnp.einsum("mrt,tc->mrc", pick_all, gated, preferred_element_type=jnp.float32)
    routed = to_experts(routed.astype(jnp.bfloat16))
    routed = jnp.stack(routed).reshape(sp_count, tp_count, slots, head_cols)
    routed = routed.transpose(1, 0, 2, 3).reshape(tp_count * sp_count * slots, head_cols)
    routed = ordered(gather_near(routed, 1), tp_index)
    routed = jnp.concatenate(routed, axis=1)
    near_rows = sp_count * slots
    routed = jnp.concatenate(
        [
            lax.dynamic_slice_in_dim(routed, (tp_index ^ m) * near_rows, near_rows, 0)
            for m in near_order(tp_count)
        ],
        axis=0,
    ).astype(jnp.float32)
    scale = lax.rsqrt(jnp.mean(routed * routed, axis=1, keepdims=True) + EPS)
    normed = (routed * scale * modulated_rescaling_vector[None, :]).astype(jnp.bfloat16)
    residual = carried[:, :model_width].astype(jnp.float32)
    middle = (
        residual + jnp.dot(normed, blender_final_matrix, preferred_element_type=jnp.float32)
    ).astype(jnp.bfloat16)
    middle_wide = middle.astype(jnp.float32)
    expert_input = (
        middle_wide
        * lax.rsqrt(jnp.mean(middle_wide * middle_wide, axis=1, keepdims=True) + EPS)
        * specialist_rescaling_vector[None, :]
    ).astype(jnp.bfloat16)

    notes = carried[:, model_width:].astype(jnp.float32)
    row_shares = notes[:, :picks] + notes[:, picks : 2 * picks]
    row_ids = notes[:, 2 * picks : 3 * picks].astype(jnp.int32) - sp_index * local_experts
    hidden = []
    for expert in range(local_experts):
        gate_value = jnp.dot(
            expert_input, specialist_gating_matrices[expert], preferred_element_type=jnp.float32
        )
        up_value = jnp.dot(
            expert_input, widening_matrices[expert], preferred_element_type=jnp.float32
        )
        share = jnp.sum(jnp.where(row_ids == expert, row_shares, 0.0), axis=1, keepdims=True)
        hidden.append((jax.nn.silu(gate_value) * up_value * share).astype(jnp.bfloat16))
    hidden = jnp.concatenate(hidden, axis=1)
    down = contracting_matrices.reshape(-1, model_width)
    order = near_order(tp_count)
    blocks = {
        m: jnp.dot(
            hidden[at * near_rows : (at + 1) * near_rows], down, preferred_element_type=jnp.float32
        )
        for at, m in enumerate(order)
    }
    bit = 1
    while bit < tp_count:
        away = sorted(m for m in blocks if m & bit)
        came = flipped(
            jnp.concatenate([blocks[m].astype(jnp.bfloat16) for m in away]), "tp", bit
        )
        blocks = {
            m ^ bit: blocks[m ^ bit]
            + came[at * near_rows : (at + 1) * near_rows].astype(jnp.float32)
            for at, m in enumerate(away)
        }
        bit *= 2
    first = (row_ids[:near_rows, :1] >= 0) & (row_ids[:near_rows, :1] < local_experts)
    answer = (blocks[0] + jnp.where(first, middle_wide[:near_rows], 0.0)).astype(jnp.bfloat16)
    returned = from_experts(answer.reshape(sp_count, slots, model_width))
    return lax.dot_general(
        pick_own,
        jnp.concatenate(returned, axis=0),
        (((0,), (0,)), ((), ())),
        preferred_element_type=jnp.float32,
    ).astype(jnp.bfloat16)


def solution(mesh):
    return jax.shard_map(
        per_device,
        mesh=mesh,
        in_specs=(
            P(("grp", "sp", "tp"), None),
            P(("grp", "sp"), "tp"),
            P(("grp", "sp"), "tp"),
            P(("grp", "sp"), "tp"),
            P(("grp", "sp"), "tp"),
            P(("grp", "sp"), "tp"),
            P(("grp", "sp"), "tp"),
            P("tp"),
            P(None, "tp"),
            P(None, "tp"),
            P(None, "tp"),
            P(),
            P(),
            P(),
            P("sp", None, "tp"),
            P("sp", None, "tp"),
            P("sp", "tp", None),
            P(("grp", "sp"), None),
            P(("grp", "sp", "tp"), None),
            P(("grp", "sp", "tp")),
        ),
        out_specs=P(("grp", "sp", "tp"), None),
        check_vma=False,
    )
```

```python
import functools

import jax
import jax.numpy as jnp
from jax import lax
from jax.experimental import pallas as pl
from jax.experimental.pallas import tpu as pltpu
from jax.sharding import PartitionSpec as P


HEAD_DIM = 64
STATE = 128
EGROUPS = 4
MANY = 8
TAIL = 16


EPS = 1e-06
HIGHEST = lax.Precision.HIGHEST


def shifted(x, axis, by):
    size = lax.axis_size(axis)
    return lax.ppermute(x, axis, [(i, (i + by) % size) for i in range(size)])


def flipped(x, axis, bit):
    return lax.ppermute(x, axis, [(i, i ^ bit) for i in range(lax.axis_size(axis))])


def from_behind(x, axis, by):
    size = lax.axis_size(axis)
    pairs = [(i, i + by) for i in range(size) if 0 <= i + by < size]
    return lax.ppermute(x, axis, pairs)


def from_all_behind(x):
    size, index = (lax.axis_size("sp"), lax.axis_index("sp"))
    if size <= MANY:
        return [from_behind(x, "sp", by) for by in range(1, size)]
    everything = lax.all_gather(x, "sp")
    return [
        jnp.where(index >= by, jnp.take(everything, jnp.maximum(index - by, 0), axis=0), 0)
        for by in range(1, size)
    ]


def exact_dot(a, b):
    return jnp.dot(a, b, precision=HIGHEST, preferred_element_type=jnp.float32)


def exact_dot_t(a, b):
    return lax.dot_general(
        a, b, (((1,), (1,)), ((), ())), precision=HIGHEST, preferred_element_type=jnp.float32
    )


def spread(heads, cols):
    head = lax.broadcasted_iota(jnp.int32, (heads, cols), 0)
    col = lax.broadcasted_iota(jnp.int32, (heads, cols), 1)
    first = head * HEAD_DIM
    return jnp.where((col >= first) & (col < first + HEAD_DIM), 1.0, 0.0)


def pick_kernel(blocks, slots, per_dest, dests):
    def body(start_ref, ids_ref, pick_ref):
        ids = ids_ref[...]
        picks, length = ids.shape
        rows = length // blocks
        dest = lax.broadcasted_iota(jnp.int32, (dests, length), 0) + start_ref[0]
        low = jnp.where(dest >= dests, dest - dests, dest) * per_dest
        member = jnp.zeros((dests, length), jnp.bool_)
        for k in range(picks):
            one = jnp.broadcast_to(ids[k : k + 1], (dests, length))
            member = member | ((one >= low) & (one < low + per_dest))
        before = lax.broadcasted_iota(jnp.int32, (length, length), 0)
        after = lax.broadcasted_iota(jnp.int32, (length, length), 1)
        base = jnp.zeros((1, length), jnp.int32)
        block_first = jnp.zeros((length, length), jnp.int32)
        for q in range(1, blocks):
            block_first = jnp.where(after >= q * rows, q * rows, block_first)
            base = jnp.where(
                lax.broadcasted_iota(jnp.int32, (1, length), 1) >= q * rows, q * slots, base
            )
        earlier = jnp.where((before < after) & (before >= block_first), 1.0, 0.0)
        rank = jnp.dot(
            jnp.where(member, 1.0, 0.0).astype(jnp.bfloat16),
            earlier.astype(jnp.bfloat16),
            preferred_element_type=jnp.float32,
        ).astype(jnp.int32)
        place = jnp.where(member, rank + base, -1)
        slot = lax.broadcasted_iota(jnp.int32, (blocks * slots, length), 0)
        for m in range(dests):
            hit = jnp.where(slot == place[m : m + 1], 1.0, 0.0)
            pick_ref[m * blocks * slots : (m + 1) * blocks * slots, :] = hit.astype(jnp.bfloat16)

    return body


def pick_rows(ids_t, start, blocks, slots, per_dest, dests):
    length = ids_t.shape[1]
    return pl.pallas_call(
        pick_kernel(blocks, slots, per_dest, dests),
        out_shape=jax.ShapeDtypeStruct((dests * blocks * slots, length), jnp.bfloat16),
        in_specs=[pl.BlockSpec(memory_space=pltpu.SMEM), pl.BlockSpec(memory_space=pltpu.VMEM)],
        name="pick_rows",
    )(start, ids_t)


def tail_body(x_ref, b_ref, c_ref, out_ref):
    width, entries = (x_ref.shape[1], b_ref.shape[1])
    out_ref[:, :width] = x_ref[...]
    out_ref[:, width : width + entries] = b_ref[...]
    out_ref[:, width + entries :] = c_ref[...]


def tails(x, keys, queries):
    length = x.shape[0]
    return pl.pallas_call(
        tail_body,
        grid=(1,),
        in_specs=[
            pl.BlockSpec((TAIL, v.shape[1]), lambda i: (length // TAIL - 1, 0))
            for v in (x, keys, queries)
        ],
        out_specs=pl.BlockSpec((TAIL, x.shape[1] + 2 * keys.shape[1]), lambda i: (0, 0)),
        out_shape=jax.ShapeDtypeStruct((TAIL, x.shape[1] + 2 * keys.shape[1]), x.dtype),
        name="tails",
    )(x, keys, queries)


def conv_of(value_ref, tail, taps_ref, scratch_ref):
    length, cols = value_ref.shape
    taps = taps_ref[...]
    kernel_len = taps.shape[0]
    scratch_ref[:TAIL, :cols] = tail
    scratch_ref[TAIL:, :cols] = value_ref[...].astype(jnp.float32)
    total = jnp.zeros((length, cols), jnp.float32)
    for offset in range(kernel_len):
        first = TAIL - kernel_len + 1 + offset
        total = total + taps[offset : offset + 1] * scratch_ref[first : first + length, :cols]
    return total * jax.nn.sigmoid(total)


def states_body(
    x_ref, b_ref, c_ref, tail_ref, raw_ref, extra_ref, rate_ref, xt_ref, bt_ref, ct_ref,
    packed_ref, scaled_ref, keys_ref, queries_ref, run_ref, run_t_ref, grown_ref, scratch_ref,
):
    length, cols = x_ref.shape
    entries = b_ref.shape[1]
    groups = entries // STATE
    heads = raw_ref.shape[0]
    tail = tail_ref[...].astype(jnp.float32)
    inputs_x = conv_of(x_ref, tail[:, :cols], xt_ref, scratch_ref)
    keys = conv_of(b_ref, tail[:, cols : cols + entries], bt_ref, scratch_ref)
    queries_ref[...] = conv_of(c_ref, tail[:, cols + entries :], ct_ref, scratch_ref)
    keys_ref[...] = keys
    raw = raw_ref[...]
    stride = jnp.maximum(raw, 0.0) + jnp.log1p(jnp.exp(-jnp.abs(raw)))
    logs = extra_ref[...] - rate_ref[...] * stride
    row = lax.broadcasted_iota(jnp.int32, (length, length), 0)
    col = lax.broadcasted_iota(jnp.int32, (length, length), 1)
    running = exact_dot_t(jnp.where(row >= col, 1.0, 0.0), logs)
    run_ref[...] = running
    run_t_ref[...] = exact_dot(logs, jnp.where(row <= col, 1.0, 0.0))
    stride = exact_dot_t(jnp.where(row == col, 1.0, 0.0), stride)
    wide = spread(heads, cols)
    scaled = inputs_x * exact_dot(stride, wide)
    scaled_ref[...] = scaled
    grown_ref[...] = exact_dot(jnp.exp(running), wide)
    last = running[length - 1 :]
    remain = exact_dot(jnp.exp(last - running), wide)
    left = scaled * remain
    width = cols // groups
    for g in range(groups):
        packed_ref[:STATE, g * width : (g + 1) * width] = exact_dot(
            keys[:, g * STATE : (g + 1) * STATE].T, left[:, g * width : (g + 1) * width]
        ).astype(jnp.bfloat16)
    decay = exact_dot(jnp.broadcast_to(jnp.exp(last), (TAIL, heads)), wide)
    packed_ref[STATE:, :] = decay.astype(jnp.bfloat16)


def inside_body(scaled_ref, keys_ref, queries_ref, run_ref, run_t_ref, out_ref):
    length, cols = scaled_ref.shape
    heads = run_ref.shape[1]
    groups = keys_ref.shape[1] // STATE
    per_group = heads // groups
    scaled = scaled_ref[...]
    running = run_ref[...]
    running_t = run_t_ref[...]
    row = lax.broadcasted_iota(jnp.int32, (length, length), 0)
    col = lax.broadcasted_iota(jnp.int32, (length, length), 1)
    lower = row >= col
    wide = spread(heads, cols)
    total = jnp.zeros((length, cols), jnp.float32)
    for g in range(groups):
        scores = lax.dot_general(
            queries_ref[:, g * STATE : (g + 1) * STATE],
            keys_ref[:, g * STATE : (g + 1) * STATE],
            (((1,), (1,)), ((), ())),
            precision=HIGHEST,
            preferred_element_type=jnp.float32,
        )
        for h in range(g * per_group, (g + 1) * per_group):
            between = running[:, h : h + 1] - running_t[h : h + 1]
            decays = jnp.exp(jnp.where(lower, between, -jnp.inf))
            total = total + exact_dot(scores * decays, scaled * wide[h : h + 1])
    out_ref[...] = total


def gate_body(pieces, inside_ref, queries_ref, grown_ref, gate_ref, pick_ref, *rest):
    behind, out_refs, gated_ref = (rest[:pieces], rest[pieces:-1], rest[-1])
    _, cols = inside_ref.shape
    groups = queries_ref.shape[1] // STATE
    width = cols // groups
    total = jnp.zeros((STATE, cols), jnp.float32)
    for piece in reversed(behind):
        decay = piece[STATE:, :].astype(jnp.float32)[:1]
        total = total * decay + piece[:STATE, :].astype(jnp.float32)
    gate = gate_ref[...].astype(jnp.float32)
    gate = gate * jax.nn.sigmoid(gate)
    for g in range(groups):
        part = slice(g * width, (g + 1) * width)
        outside = exact_dot(queries_ref[:, g * STATE : (g + 1) * STATE], total[:, part])
        gated_ref[:, part] = (
            (inside_ref[:, part] + outside * grown_ref[:, part]) * gate[:, part]
        ).astype(jnp.bfloat16)
    gated = gated_ref[...]
    size = out_refs[0].shape[0]
    for m, out_ref in enumerate(out_refs):
        out_ref[...] = jnp.dot(
            pick_ref[m * size : (m + 1) * size, :], gated, preferred_element_type=jnp.float32
        ).astype(jnp.bfloat16)


def sp_exchange(pieces, sign):
    size, index = (lax.axis_size("sp"), lax.axis_index("sp"))
    if size <= MANY:
        return [pieces[0]] + [shifted(pieces[m], "sp", sign * m) for m in range(1, size)]
    places = jnp.arange(size, dtype=jnp.int32)
    sent = jnp.take(jnp.stack(list(pieces)), (sign * (places - index)) % size, axis=0)
    came = lax.all_to_all(sent, "sp", split_axis=0, concat_axis=0, tiled=True)
    came = jnp.take(came, (index - sign * places) % size, axis=0)
    return [came[m] for m in range(size)]


def to_experts(pieces):
    return sp_exchange(pieces, 1)


def near_order(size):
    order, bit = ([0], size // 2)
    while bit:
        order = order + [m | bit for m in order]
        bit //= 2
    return order


def gather_near(blocks, axis):
    bit, width = (lax.axis_size("tp") // 2 // len(blocks), blocks[0].shape[axis])
    while bit:
        came = flipped(jnp.concatenate(blocks, axis=axis), "tp", bit)
        blocks = blocks + [
            lax.slice_in_dim(came, i * width, (i + 1) * width, axis=axis)
            for i in range(len(blocks))
        ]
        bit //= 2
    return blocks


def ordered(blocks, index):
    by = dict(zip(near_order(len(blocks)), blocks))
    bit = 1
    while bit < len(blocks):
        here = (index & bit) != 0
        by = {m: jnp.where(here, by[m ^ bit], by[m]) for m in by}
        bit *= 2
    return [by[m] for m in range(len(blocks))]


def layer(
    carryover_vector,
    channel_source_entries,
    final_modulation_vector,
    entering_basis_matrix,
    readout_basis_matrix,
    raw_stride_amount,
    extra_log_attenuation,
    channel_fading_rate,
    channel_source_kernel,
    entering_basis_kernel,
    readout_basis_kernel,
    modulated_rescaling_vector,
    blender_final_matrix,
    specialist_rescaling_vector,
    specialist_gating_matrices,
    widening_matrices,
    contracting_matrices,
    assigned_specialist_ids,
    specialist_choice_affinity,
    cluster_chance,
):
    length, head_cols = channel_source_entries.shape
    row_count, model_width = carryover_vector.shape
    heads_here = channel_fading_rate.shape[0]
    state_cols = entering_basis_matrix.shape[1]
    sp_count, sp_index = (lax.axis_size("sp"), lax.axis_index("sp"))
    tp_count, tp_index = (lax.axis_size("tp"), lax.axis_index("tp"))
    local_experts = specialist_gating_matrices.shape[0]
    experts = sp_count * local_experts
    picks = assigned_specialist_ids.shape[1]
    capacity = 2 * row_count * picks // experts
    slots = min(local_experts * capacity, capacity * (experts // EGROUPS) // picks)

    tail = tails(channel_source_entries, entering_basis_matrix, readout_basis_matrix)
    tail, routing_ids = lax.optimization_barrier((tail, assigned_specialist_ids))
    neighbours = from_behind(tail, "sp", 1)

    start = sp_index.astype(jnp.int32).reshape(1)
    own_ids = lax.dynamic_slice_in_dim(routing_ids, tp_index * row_count, row_count, 0)
    pick_own = pick_rows(own_ids.T, start, 1, slots, local_experts, sp_count)
    pick_all = pick_rows(
        routing_ids.T, start, tp_count, slots, local_experts, sp_count
    )

    lifted = jnp.exp(specialist_choice_affinity)
    shares = cluster_chance[:, None] * lifted / jnp.sum(lifted, axis=1, keepdims=True)
    shares_high = shares.astype(jnp.bfloat16)
    shares_low = (shares - shares_high.astype(jnp.float32)).astype(jnp.bfloat16)
    notes = jnp.concatenate([shares_high, shares_low, own_ids.astype(jnp.bfloat16)], axis=1)
    notes = jnp.pad(notes, ((0, 0), (0, 128 - 3 * picks)))
    early = jnp.dot(
        pick_own,
        jnp.concatenate([carryover_vector, notes], axis=1),
        preferred_element_type=jnp.float32,
    ).astype(jnp.bfloat16)
    early = to_experts(early.reshape(sp_count, slots, model_width + 128))

    segment = jax.ShapeDtypeStruct((length, head_cols), jnp.float32)
    state_map = jax.ShapeDtypeStruct((length, state_cols), jnp.float32)
    packed, scaled, keys_b, queries_c, running, running_t, grown = pl.pallas_call(
        states_body,
        out_shape=(
            jax.ShapeDtypeStruct((STATE + TAIL, head_cols), jnp.bfloat16),
            segment,
            state_map,
            state_map,
            jax.ShapeDtypeStruct((length, heads_here), jnp.float32),
            jax.ShapeDtypeStruct((heads_here, length), jnp.float32),
            segment,
        ),
        scratch_shapes=[pltpu.VMEM((length + TAIL, max(head_cols, state_cols)), jnp.float32)],
        name="states",
    )(
        channel_source_entries,
        entering_basis_matrix,
        readout_basis_matrix,
        neighbours,
        raw_stride_amount.T,
        extra_log_attenuation.T,
        channel_fading_rate[:, None],
        channel_source_kernel,
        entering_basis_kernel,
        readout_basis_kernel,
    )
    packed, *early = lax.optimization_barrier((packed, *early))
    halves = (
        list(range(1, sp_count // 2 + 1)),
        list(range(sp_count // 2 + 1, sp_count)) + [0],
    )
    early = jnp.concatenate([early[m] for half in halves for m in half], axis=0)
    near_x = flipped(early, "tp", tp_count // 2)
    behind = from_all_behind(packed)
    inside = pl.pallas_call(inside_body, out_shape=segment, name="inside")(
        scaled, keys_b, queries_c, running, running_t
    )
    routed = pl.pallas_call(
        functools.partial(gate_body, len(behind)),
        out_shape=[
            jax.ShapeDtypeStruct((tp_count * slots, head_cols), jnp.bfloat16)
            for _ in range(sp_count)
        ],
        scratch_shapes=[pltpu.VMEM((length, head_cols), jnp.bfloat16)],
        name="gate",
    )(inside, queries_c, grown, final_modulation_vector, pick_all, *behind)

    routed = to_experts(routed)
    *routed, near_x = lax.optimization_barrier((*routed, near_x))
    carried = gather_near([early, near_x], 0)
    ends = [0]
    for half in halves:
        ends.append(ends[-1] + len(half) * slots)
    carried = jnp.concatenate(
        [block[lo:hi] for lo, hi in zip(ends, ends[1:]) for block in carried], axis=0
    )
    routed = jnp.concatenate(
        [
            jnp.stack([routed[m].reshape(tp_count, slots, head_cols) for m in half], axis=1)
            .reshape(tp_count * len(half) * slots, head_cols)
            for half in halves
        ]
    )
    routed = ordered(gather_near([routed], 1), tp_index)
    routed = jnp.concatenate(routed, axis=1)
    order = near_order(tp_count)
    sizes = [len(half) * slots for half in halves]
    routed = jnp.concatenate(
        [
            lax.dynamic_slice_in_dim(routed, tp_count * lo + (tp_index ^ m) * size, size, 0)
            for lo, size in zip(ends, sizes)
            for m in order
        ],
        axis=0,
    ).astype(jnp.float32)
    scale = lax.rsqrt(jnp.mean(routed * routed, axis=1, keepdims=True) + EPS)
    normed = (routed * scale * modulated_rescaling_vector[None, :]).astype(jnp.bfloat16)
    residual = carried[:, :model_width].astype(jnp.float32)
    middle = (
        residual + jnp.dot(normed, blender_final_matrix, preferred_element_type=jnp.float32)
    ).astype(jnp.bfloat16)
    middle_wide = middle.astype(jnp.float32)
    expert_input = (
        middle_wide
        * lax.rsqrt(jnp.mean(middle_wide * middle_wide, axis=1, keepdims=True) + EPS)
        * specialist_rescaling_vector[None, :]
    ).astype(jnp.bfloat16)

    notes = carried[:, model_width:].astype(jnp.float32)
    row_shares = notes[:, :picks] + notes[:, picks : 2 * picks]
    row_ids = notes[:, 2 * picks : 3 * picks].astype(jnp.int32) - sp_index * local_experts
    hidden = []
    for expert in range(local_experts):
        gate_value = jnp.dot(
            expert_input, specialist_gating_matrices[expert], preferred_element_type=jnp.float32
        )
        up_value = jnp.dot(
            expert_input, widening_matrices[expert], preferred_element_type=jnp.float32
        )
        share = jnp.sum(jnp.where(row_ids == expert, row_shares, 0.0), axis=1, keepdims=True)
        hidden.append((jax.nn.silu(gate_value) * up_value * share).astype(jnp.bfloat16))
    hidden = jnp.concatenate(hidden, axis=1)
    down = contracting_matrices.reshape(-1, model_width)
    returned = [None] * sp_count
    for lo, size, half in zip(ends, sizes, halves):
        base = tp_count * lo
        blocks = {
            m: jnp.dot(
                hidden[base + at * size : base + (at + 1) * size],
                down,
                preferred_element_type=jnp.float32,
            )
            for at, m in enumerate(order)
        }
        bit = 1
        while bit < tp_count:
            away = sorted(m for m in blocks if m & bit)
            came = flipped(
                jnp.concatenate([blocks[m].astype(jnp.bfloat16) for m in away]), "tp", bit
            )
            blocks = {
                m ^ bit: blocks[m ^ bit] + came[at * size : (at + 1) * size].astype(jnp.float32)
                for at, m in enumerate(away)
            }
            bit *= 2
        first = row_ids[base : base + size, :1]
        first = (first >= 0) & (first < local_experts)
        answer = blocks[0] + jnp.where(first, middle_wide[base : base + size], 0.0)
        answer = answer.astype(jnp.bfloat16).reshape(len(half), slots, model_width)
        for at, m in enumerate(half):
            if sp_count <= MANY and m:
                returned[m] = shifted(answer[at], "sp", -m)
            else:
                returned[m] = answer[at]
    if sp_count > MANY:
        returned = sp_exchange(returned, -1)
    return lax.dot_general(
        pick_own,
        jnp.concatenate(returned, axis=0),
        (((0,), (0,)), ((), ())),
        preferred_element_type=jnp.float32,
    ).astype(jnp.bfloat16)


def solution(mesh):
    return jax.shard_map(
        layer,
        mesh=mesh,
        in_specs=(
            P(("grp", "sp", "tp"), None),
            P(("grp", "sp"), "tp"),
            P(("grp", "sp"), "tp"),
            P(("grp", "sp"), "tp"),
            P(("grp", "sp"), "tp"),
            P(("grp", "sp"), "tp"),
            P(("grp", "sp"), "tp"),
            P("tp"),
            P(None, "tp"),
            P(None, "tp"),
            P(None, "tp"),
            P(),
            P(),
            P(),
            P("sp", None, "tp"),
            P("sp", None, "tp"),
            P("sp", "tp", None),
            P(("grp", "sp"), None),
            P(("grp", "sp", "tp"), None),
            P(("grp", "sp", "tp")),
        ),
        out_specs=P(("grp", "sp", "tp"), None),
        check_vma=False,
    )
```
